32 devices in a mesh: grp: 2 (over y), fs: 4 (over z), tp: 4 (over x, core).
Axes of the slice: x: 2, y: 2, z: 4, core: 2. Of those that a mesh axis runs over, the one named last changes fastest.
Arguments:
- prompt: bfloat16 [1024, 2048], P(('grp', 'fs', 'tp')), parts along dimension 0, may hold values from -6 to 6
- norm_gain: float32 [2048], P('fs'), may hold values from 0.1 to 1.9
- up_weight: float32 [2048, 8192], P('fs', 'tp'), may hold values from -0.125 to 0.125
- down_weight: float32 [8192, 2048], P('fs', 'tp'), may hold values from -0.0625 to 0.0625
Outputs:
- up_serving: bfloat16 [4096, 8192], P('grp', 'fs'), parts along dimension 0
- down_serving: bfloat16 [8192, 4096], P('fs', 'grp'), parts along dimension 1
- mlp_output: bfloat16 [1024, 2048], P(('grp', 'fs', 'tp')), parts along dimension 0
The draws below stay inside these ranges and needn't reach their ends.
There are 2 independent parts, one for each index of `grp`. The reference program is written for one: setup_inputs(seed, part) draws one part's arguments, and reference() takes and returns one part's arrays. A program takes and returns all parts, laid end to end along the dimension named above; an argument that names none is the same for every part. Nothing has to cross between parts.
All inputs are finite; a program needn't handle non-finite values.
Results may differ from the reference program's by a relative error of at most 0.024.
Values may be sent and summed in bfloat16 or wider, within the bound.
A program may use at most 128 MiB of HBM per device.

```python
import jax
import jax.numpy as jnp
from jax import lax

D = 2048
FF = 8192
TOKENS = 512
UNITS_DEV = 2048
N_FS = 4


def level_of(key, dims, cuts, least, top_value):
    def one(position, blocks):
        heights = jax.random.uniform(jax.random.fold_in(jax.random.fold_in(key, 6), position), (blocks,), jnp.float32, least / len(cuts), top_value / len(cuts))
        return jnp.repeat(jnp.exp(heights), dims[position] // blocks).reshape((-1,) + (1,) * (len(dims) - position - 1))

    factor_of = one(*cuts[0])
    for cut in cuts[1:]:
        factor_of = factor_of * one(*cut)
    return factor_of


def gaussian(rng, dims, spread, reach, shards=(), kind=jnp.bfloat16):
    array = jax.random.normal(rng, dims, jnp.float32) * spread
    if len(shards) > 0:
        array = level_of(rng, dims, shards, -0.22, 0.18) * array
    return jnp.clip(array, min=-reach, max=reach).astype(kind)


def setup_inputs(seed: int = 0, part: int = 0) -> dict:
    keys = jax.random.split(jax.random.key(seed), 5)
    part_keys = jax.random.split(jax.random.fold_in(keys[4], part), 5)
    return {
        "prompt": gaussian(part_keys[0], (TOKENS, D), 1.0, 6.0, ((0, 16),)),
        "norm_gain": jnp.clip(1.0 + 0.18 * jax.random.normal(keys[1], (D,), jnp.float32), 0.1, 1.9),
        "up_weight": gaussian(keys[2], (D, FF), D ** -0.5, 0.125, ((0, 4), (1, 4)), jnp.float32),
        "down_weight": gaussian(keys[3], (FF, D), FF ** -0.5, 0.0625, ((0, 4), (1, 4)), jnp.float32),
    }


epsilon = 1e-06

def reference(prompt, norm_gain, up_weight, down_weight):
    up_serving = (norm_gain[:, None] * up_weight).astype(jnp.bfloat16)
    down_serving = down_weight.astype(jnp.bfloat16)
    widened = prompt.astype(jnp.float32)
    normed = (widened * lax.rsqrt(lax.optimization_barrier(jnp.mean(widened * widened, axis=-1, keepdims=True)) + epsilon)).astype(jnp.bfloat16)
    projected = jnp.dot(normed, up_serving, preferred_element_type=jnp.float32)
    hidden = jnp.square(jax.nn.relu(projected)).astype(jnp.bfloat16)

    def add_block(summed, block_index):
        offset = (block_index * UNITS_DEV).astype(jnp.int32)
        col_block = lax.dynamic_slice_in_dim(hidden, offset, UNITS_DEV, 1)
        row_block = lax.dynamic_slice_in_dim(down_serving, offset, UNITS_DEV, 0)
        partial_value = jnp.dot(col_block, row_block, preferred_element_type=jnp.float32).astype(jnp.bfloat16)
        partial_value = lax.optimization_barrier(partial_value)
        return (summed + partial_value.astype(jnp.float32), None)
    summed, _ = lax.scan(add_block, jnp.zeros((prompt.shape[0], down_serving.shape[1]), jnp.float32), jnp.arange(N_FS, dtype=jnp.int32))
    return (up_serving, down_serving, summed.astype(jnp.bfloat16))
```

```python
import functools

import jax
import jax.numpy as jnp
from jax import lax
from jax.experimental import pallas as pl
from jax.experimental.pallas import tpu as pltpu
from jax.sharding import PartitionSpec as P

epsilon = 1e-06
CORES = 2
PIECES = 4
UP_STEPS = 8
READS = 4
LANES = 128
K_PIECES = 4
WHOLE_PART = 0.5
AHEAD = 2
STAGE = (0.05, 0.45)
ARRIVAL = ((0.06, 0.52), (0.13, 0.55), (0.18, 0.78), (0.22, 1.02))
LAG_Y = 0.2
ROWS = (0.12, 0.6)
MESH = pl.DeviceIdType.MESH


def rank(origin, at, count):
    half = count // 2
    far = (origin < half) != (at < half)
    inner = abs(2 * origin - count + 1)
    if abs(2 * at - count + 1) > 1:
        return (far, -inner)
    return (-inner, not far)


def kernel(
    groups, fs_count, tp_count, up_steps, whole_cols, k_pieces,
    gain, up_w, down_w, prompt, up_v, down_v, out_v,
    gain_v, prompt_v, up_f, down_f, gain_col,
    ub, nb, nall, proj, hidden, pbuf, rbuf, stage,
    in_sem, up_send, stage_recv, z_send, up_recv, upf_send, own_send, own_recv,
    dn_send, dn_recv, dnf_send, sib_send, sib_recv,
    n_send, n_recv, r_send, r_recv,
):
    y, z, t = lax.axis_index("grp"), lax.axis_index("fs"), lax.axis_index("tp")
    x, c = t // CORES, lax.rem(t, CORES)
    chips = tp_count // CORES
    ratio, rows, units = ub.shape
    chunk = rows // (up_steps * CORES * groups)
    width = down_w.shape[1]
    col_chunks = width // LANES
    k_rows = units // k_pieces
    tokens = prompt.shape[0]
    sibling = (y, z, x * CORES + 1 - c)
    t_src = z // ratio
    x_src, c_src = t_src // CORES, lax.rem(t_src, CORES)
    same_x = x == x_src

    up_part = rows // READS
    down_part = units // READS

    def up_read(i):
        at = pl.ds(i * up_part, up_part)
        return pltpu.make_async_copy(up_w.at[at, :], up_f.at[at, :], in_sem.at[2 + i])

    def down_read(i):
        at = pl.ds(i * down_part, down_part)
        return pltpu.make_async_copy(down_w.at[at, :], down_f.at[at, :], in_sem.at[2 + READS + i])

    gain_read = pltpu.make_async_copy(gain, gain_v, in_sem.at[0])
    prompt_read = pltpu.make_async_copy(prompt, prompt_v, in_sem.at[1])
    gain_read.start()
    prompt_read.start()
    for i in range(READS):
        up_read(i).start()
    for i in range(READS):
        down_read(i).start()

    barrier = pltpu.get_barrier_semaphore()
    peers = [sibling]
    peers += [(y, lax.rem(z + d, fs_count), x * CORES + cc) for d in range(1, fs_count) for cc in range(CORES)]
    peers += [(y, z, lax.rem(x + d, chips) * CORES + cc) for d in range(1, chips) for cc in range(CORES)]
    peers += [(lax.rem(y + g, groups), z, t) for g in range(1, groups)]
    for peer in peers:
        pl.semaphore_signal(barrier, inc=1, device_id=peer, device_id_type=MESH)

    gain_read.wait()
    gain_col[...] = jnp.broadcast_to(gain_v[...], (LANES, rows)).T
    prompt_read.wait()
    widened = prompt_v[...].astype(jnp.float32)
    scale = lax.rsqrt(jnp.mean(widened * widened, axis=-1, keepdims=True) + epsilon)
    nb[...] = (widened * scale).astype(jnp.bfloat16)
    step = min(16, up_part)
    for n in range(READS):
        up_read(n).wait()

        @pl.loop(0, up_part // step)
        def _(i):
            at = pl.ds(pl.multiple_of(n * up_part + i * step, step), step)
            factor = gain_col[at, :]
            for j in range(ratio):
                for b in range(units // LANES):
                    piece = up_f[at, j * units + b * LANES : j * units + (b + 1) * LANES]
                    ub[j, at, b * LANES : (b + 1) * LANES] = (factor * piece).astype(jnp.bfloat16)

    pl.semaphore_wait(barrier, len(peers))

    def remote(src, dst, ssem, rsem, dev):
        return pltpu.make_async_remote_copy(
            src_ref=src, dst_ref=dst, send_sem=ssem, recv_sem=rsem, device_id=dev, device_id_type=MESH
        )

    def n_at(zr):
        return nall.at[pl.ds(pl.multiple_of(zr * tokens, tokens), tokens), :]

    def n_copy(zr, up, first):
        src = nb if first else n_at(zr)
        dev = (y, z + 1 if up else z - 1, t)
        return remote(src, n_at(zr), n_send.at[zr, int(up)], n_recv.at[zr], dev)

    def n_hop(h, act, wait):
        for up in (True, False):
            origin = z - h if up else z + h

            @pl.when(jnp.logical_and(origin >= 0, origin < fs_count))
            def _():
                if wait and h > 0:
                    remote(nb, n_at(origin), n_send.at[origin, int(up)], n_recv.at[origin], sibling).wait_recv()

                @pl.when(z < fs_count - 1 if up else z > 0)
                def _():
                    act(n_copy(origin, up, h == 0))

    def up_at(zr, k):
        return up_v.at[pl.ds(pl.multiple_of(zr * rows + k * chunk, chunk), chunk), :]

    def up_index(m, core, owner):
        return (m * CORES + core) * groups + owner

    def src_at(j, m, cd):
        k = up_index(m, cd, y)
        return ub.at[j, pl.ds(pl.multiple_of(k * chunk, chunk), chunk), :]

    def up_x(j, m, cd, dx):
        dev = (y, z, lax.rem(x + dx, chips) * CORES + c)
        sem = up_send.at[j, m, cd, dx]
        return remote(src_at(j, m, cd), stage.at[x, j, m, cd], sem, stage_recv.at[x, j, m, cd], dev)

    def up_x_own(j, m, cd, dx):
        dev = (y, z, lax.rem(x + dx, chips) * CORES + cd)
        k = up_index(m, cd, y)
        return remote(src_at(j, m, cd), up_at(z, k), up_send.at[j, m, cd, dx], up_recv.at[z, k], dev)

    def up_x_all(act):
        for m in range(up_steps):
            for cd in range(CORES):
                for j in range(ratio):
                    mine = t * ratio + j == z
                    for dx in range(1, chips):
                        @pl.when(mine)
                        def _():
                            act(up_x_own(j, m, cd, dx))

                        @pl.when(jnp.logical_not(mine))
                        def _():
                            act(up_x(j, m, cd, dx))

    def up_z(j, m, cd, dx):
        xs = lax.rem(x + dx, chips)
        src = src_at(j, m, cd) if dx == 0 else stage.at[xs, j, m, cd]
        k = up_index(m, cd, y)
        dev = (y, (xs * CORES + c) * ratio + j, x * CORES + cd)
        return remote(src, up_at(z, k), z_send.at[j, m, cd, dx], up_recv.at[z, k], dev)

    def up_z_one(j, m, cd, dx, act):
        xs = lax.rem(x + dx, chips)

        @pl.when((xs * CORES + c) * ratio + j != z)
        def _():
            act(j, m, cd, dx)

    def go_z(j, m, cd, dx):
        if dx > 0:
            xs = lax.rem(x + dx, chips)
            at = stage.at[xs, j, m, cd]
            remote(at, at, up_send.at[j, m, cd, dx], stage_recv.at[xs, j, m, cd], sibling).wait_recv()
        up_z(j, m, cd, dx).start()

    def z_own(m):
        for cd in range(CORES):
            for j in range(ratio):
                up_z_one(j, m, cd, 0, go_z)

    def z_staged(m):
        for cd in range(CORES):
            for j in range(ratio):
                for dx in range(1, chips):
                    up_z_one(j, m, cd, dx, go_z)

    own_j = lax.rem(z, ratio)
    own_rows = pl.ds(pl.multiple_of(z * rows, rows), rows)
    my_cols = pl.ds(pl.multiple_of(t * width, width), width)

    def own_copy():
        return remote(ub.at[own_j], up_v.at[own_rows, :], own_send, own_recv, sibling)

    def sib_copy():
        return remote(down_v.at[:, my_cols], down_v.at[:, my_cols], sib_send, sib_recv, sibling)

    def cols_of(ts, i):
        return pl.ds(pl.multiple_of(ts * width + i * LANES, LANES), LANES)

    def dn_at(ts, i, k):
        return down_v.at[pl.ds(pl.multiple_of(k * k_rows, k_rows), k_rows), cols_of(ts, i)]

    def dn_first(i, k, dx):
        dev = (y, z, lax.rem(x + dx, chips) * CORES + c)
        return remote(dn_at(t, i, k), dn_at(t, i, k), dn_send.at[i, k, dx], dn_recv.at[t, i, k], dev)

    def dn_sends(act):
        for i in range(col_chunks):
            if i < whole_cols:
                for k in range(k_pieces):
                    for dx in range(1, chips):
                        act(dn_first(i, k, dx))
            else:
                for n in range(k_pieces // groups):
                    for dx in range(1, chips):
                        act(dn_first(i, n * groups + y, dx))

    start = lambda copy: copy.start()
    n_hop(0, start, False)
    for m in range(min(AHEAD, up_steps)):
        z_own(m)
    up_x_all(start)

    @pl.when(t == t_src)
    def _():
        own_copy().start()

    down_step = min(64, down_part)
    for n in range(READS):
        down_read(n).wait()

        @pl.loop(0, down_part // down_step)
        def _(i):
            at = pl.ds(pl.multiple_of(n * down_part + i * down_step, down_step), down_step)
            down_v[at, my_cols] = down_f[at, :].astype(jnp.bfloat16)

    dn_sends(start)
    sib_copy().start()

    n_at(z)[...] = nb[...]

    @pl.when(t == t_src)
    def _():
        @pl.loop(0, rows // chunk)
        def _(i):
            part = pl.ds(pl.multiple_of(i * chunk, chunk), chunk)
            up_v[pl.ds(pl.multiple_of(z * rows + i * chunk, chunk), chunk), :] = ub[own_j, part, :]

    def up_y(zr, k, g):
        dev = (lax.rem(y + g, groups), z, t)
        return remote(up_at(zr, k), up_at(zr, k), upf_send.at[zr, k, g], up_recv.at[zr, k], dev)

    def up_s(zr, k):
        return remote(up_at(zr, k), up_at(zr, k), upf_send.at[zr, k, 0], up_recv.at[zr, k], sibling)

    def dn_y(ts, i, k, g):
        dev = (lax.rem(y + g, groups), z, t)
        return remote(dn_at(ts, i, k), dn_at(ts, i, k), dnf_send.at[ts, i, k, g], dn_recv.at[ts, i, k], dev)

    def dn_s(ts, i, k):
        return remote(dn_at(ts, i, k), dn_at(ts, i, k), dnf_send.at[ts, i, k, 0], dn_recv.at[ts, i, k], sibling)

    def if_remote(d, fn):
        if d == 0:
            pl.when(jnp.logical_not(same_x))(fn)
        else:
            fn()

    def source(d):
        if d == 0 or fs_count > 8:
            return lax.rem(z + d, fs_count)
        found = 0
        for at in range(fs_count):
            order = sorted((o for o in range(fs_count) if o != at), key=lambda o: rank(o, at, fs_count))
            found = jnp.where(z == at, order[d - 1], found)
        return found

    def up_a(m, d):
        def go():
            zr, k = source(d), up_index(m, c, y)
            up_s(zr, k).wait_recv()
            for g in range(1, groups):
                up_y(zr, k, g).start()
            up_s(zr, k).start()

        if_remote(d, go)

    def up_b(m, d):
        def go():
            zr = source(d)
            for g in range(1, groups):
                k = up_index(m, c, lax.rem(y + g, groups))
                up_s(zr, k).wait_recv()
                up_s(zr, k).start()

        if_remote(d, go)

    def up_c(d):
        def go():
            zr = source(d)
            for m in range(up_steps):
                for owner in range(groups):
                    up_s(zr, up_index(m, 1 - c, owner)).wait_recv()

        if_remote(d, go)

    def up_f(d):
        def go():
            zr = source(d)
            for m in range(up_steps):
                for owner in range(groups):
                    up_s(zr, up_index(m, c, owner)).wait_send()
                for g in range(1, groups):
                    up_y(zr, up_index(m, c, y), g).wait_send()

        if_remote(d, go)

    def dn_src(dx):
        return lax.rem(x + dx, chips) * CORES + c

    def dn_one(i, k, dx):
        ts = dn_src(dx)
        dn_s(ts, i, k).wait_recv()
        dn_s(ts, i, k).start()

    def dn_a(i, n, dx):
        ts, k = dn_src(dx), n * groups + y
        dn_s(ts, i, k).wait_recv()
        for g in range(1, groups):
            dn_y(ts, i, k, g).start()
        dn_s(ts, i, k).start()

    def dn_b(i, n, dx):
        for g in range(1, groups):
            dn_one(i, n * groups + lax.rem(y + g, groups), dx)

    part = functools.partial
    events = []
    for m in range(up_steps):
        share = m / max(1, up_steps - 1)
        when = STAGE[0] + (STAGE[1] - STAGE[0]) * share
        events.append((when, part(z_staged, m)))
        if m + AHEAD < up_steps:
            events.append((when + 0.001, part(z_own, m + AHEAD)))
        for d in range(fs_count):
            base, span = ARRIVAL[min(d, len(ARRIVAL) - 1)]
            when = max(base + (span - base) * share, STAGE[0] + (STAGE[1] - STAGE[0]) * share + 0.01) + 0.002 * d
            events.append((when, part(up_a, m, d)))
            events.append((when + LAG_Y, part(up_b, m, d)))
    for h in range(1, fs_count):
        when = ROWS[h - 1] if h <= len(ROWS) else 1.2 + h
        events.append((when, part(n_hop, h, start, True)))
    for i in range(whole_cols):
        for dx in range(1, chips):
            for k in range(k_pieces):
                events.append((1.1, part(dn_one, i, k, dx)))
    for _, event in sorted(events, key=lambda e: e[0]):
        event()

    for d in range(fs_count):
        up_c(d)

    @pl.when(jnp.logical_and(same_x, t != t_src))
    def _():
        own_copy().wait_recv()

    depth = prompt.shape[1]
    kb = 256
    nb_tile = min(units, 1024)

    split = range(whole_cols, col_chunks)
    rest = [part(dn_a, i, n, dx) for i in split for n in range(k_pieces // groups) for dx in range(1, chips)]
    pieces = depth // kb
    done = 0
    for i in range(pieces):
        for j in range(units // nb_tile):
            col = pl.ds(j * nb_tile, nb_tile)
            term = jnp.dot(
                nall[:, i * kb : (i + 1) * kb],
                up_v[i * kb : (i + 1) * kb, col],
                preferred_element_type=jnp.float32,
            )
            if i == 0:
                proj[:, col] = term
            else:
                proj[:, col] += term
        upto = len(rest) * (i + 1) // (2 * pieces)
        for fn in rest[done:upto]:
            fn()
        done = upto

    positive = jnp.maximum(proj[...], 0.0)
    hidden[...] = (positive * positive).astype(jnp.bfloat16)

    def r_copy(ts, i, wide, d):
        zt = lax.rem(z + d, fs_count)
        cols = pl.ds(pl.multiple_of(ts * width + i * LANES, LANES), wide)
        sems = r_send.at[ts, i, d], r_recv.at[z, ts, i]
        return remote(pbuf.at[zt, :, cols], rbuf.at[z, :, cols], *sems, (y, zt, t))

    def r_done(ts, i, wide, d):
        zr = lax.rem(z + d, fs_count)
        cols = pl.ds(pl.multiple_of(ts * width + i * LANES, LANES), wide)
        sems = r_send.at[ts, i, d], r_recv.at[zr, ts, i]
        remote(pbuf.at[zr, :, cols], rbuf.at[zr, :, cols], *sems, (y, zr, t)).wait()

    def block(ts, i, wide):
        cols = pl.ds(pl.multiple_of(ts * width + i * LANES, LANES), wide)
        part = jnp.dot(hidden[...], down_v[:, cols], preferred_element_type=jnp.float32).astype(jnp.bfloat16)
        pbuf[:, :, cols] = part.reshape(fs_count, tokens, wide)

    blocks = [(t, 0, width), (x * CORES + 1 - c, 0, width)]
    for i in range(col_chunks):
        for dx in range(1, chips):
            blocks += [(dn_src(dx), i, LANES), (lax.rem(x + dx, chips) * CORES + 1 - c, i, LANES)]

    def send_block(ts, i, wide):
        for d in range(1, fs_count):
            r_copy(ts, i, wide, d).start()

    last = None
    for index, (ts, i, wide) in enumerate(blocks):
        if index == 1:
            sib_copy().wait_recv()
        if index >= CORES:
            dx = 1 + (index - CORES) // CORES % (chips - 1)
            if (index - CORES) % CORES == 0 and i >= whole_cols:
                for n in range(k_pieces // groups):
                    dn_b(i, n, dx)
            if (index - CORES) % CORES == 1:
                for k in range(k_pieces):
                    dn_s(ts, i, k).wait_recv()
        block(ts, i, wide)
        if index < CORES:
            upto = len(rest) if index == CORES - 1 else (done + len(rest)) // 2
            for fn in rest[done:upto]:
                fn()
            done = upto
        if last is not None:
            send_block(*last)
        last = (ts, i, wide)
    send_block(*last)

    for d in range(fs_count):
        up_f(d)
    for dx in range(1, chips):
        ts = dn_src(dx)
        for i in range(col_chunks):
            for k in range(k_pieces):
                dn_s(ts, i, k).wait_send()
            if i >= whole_cols:
                for n in range(k_pieces // groups):
                    for g in range(1, groups):
                        dn_y(ts, i, n * groups + y, g).wait_send()
    up_x_all(lambda copy: copy.wait_send())
    for m in range(up_steps):
        for cd in range(CORES):
            for j in range(ratio):
                for dx in range(chips):
                    up_z_one(j, m, cd, dx, lambda *at: up_z(*at).wait_send())
    dn_sends(lambda copy: copy.wait_send())
    sib_copy().wait_send()

    @pl.when(t == t_src)
    def _():
        own_copy().wait_send()

    for h in range(fs_count):
        n_hop(h, lambda copy: copy.wait_send(), False)

    total = pbuf[z].astype(jnp.float32)
    for ts, i, wide in blocks:
        @pl.loop(1, fs_count)
        def _(d):
            r_done(ts, i, wide, d)

    for d in range(1, fs_count):
        total += rbuf[lax.rem(z + d, fs_count)].astype(jnp.float32)
    out_v[...] = total.astype(jnp.bfloat16)


def write_out(up_v, down_v, out_v, up_out, down_out, mlp_out, sems):
    copies = [pltpu.make_async_copy(out_v, mlp_out, sems.at[2 * PIECES])]
    for n, (src, dst) in enumerate(((up_v, up_out), (down_v, down_out))):
        step = src.shape[0] // PIECES
        for i in range(PIECES):
            part = pl.ds(i * step, step)
            copies.append(pltpu.make_async_copy(src.at[part, :], dst.at[part, :], sems.at[n * PIECES + i]))
    for copy in copies:
        copy.start()
    for copy in copies:
        copy.wait()


def per_device(groups, prompt, norm_gain, up_weight, down_weight):
    tp_count, fs_count = lax.axis_size("tp"), lax.axis_size("fs")
    rows, wide = up_weight.shape
    units, width = down_weight.shape
    tokens, depth = prompt.shape
    ratio = wide // units
    up_steps = max(1, min(UP_STEPS, rows // (CORES * groups * 16)))
    col_chunks = width // LANES
    whole_cols = int(col_chunks * WHOLE_PART)
    chips = tp_count // CORES
    kc = up_steps * CORES * groups
    k_pieces = K_PIECES
    f32, bf16 = jnp.float32, jnp.bfloat16
    dma = pltpu.SemaphoreType.DMA
    vmem = pl.BlockSpec(memory_space=pltpu.VMEM)
    hbm = pl.BlockSpec(memory_space=pltpu.HBM)
    up_v, down_v, out_v = pl.pallas_call(
        functools.partial(kernel, groups, fs_count, tp_count, up_steps, whole_cols, k_pieces),
        out_shape=(
            pltpu.VMEM((depth, units), bf16),
            pltpu.VMEM((units, depth), bf16),
            jax.ShapeDtypeStruct((tokens, depth), bf16),
        ),
        in_specs=[hbm] * 4,
        out_specs=(vmem,) * 3,
        scratch_shapes=[
            pltpu.VMEM((1, rows), f32),
            pltpu.VMEM((tokens, depth), bf16),
            pltpu.VMEM((rows, wide), f32),
            pltpu.VMEM((units, width), f32),
            pltpu.VMEM((rows, LANES), f32),
            pltpu.VMEM((ratio, rows, units), bf16),
            pltpu.VMEM((tokens, depth), bf16),
            pltpu.VMEM((fs_count * tokens, depth), bf16),
            pltpu.VMEM((fs_count * tokens, units), f32),
            pltpu.VMEM((fs_count * tokens, units), bf16),
            pltpu.VMEM((fs_count, tokens, depth), bf16),
            pltpu.VMEM((fs_count, tokens, depth), bf16),
            pltpu.VMEM((chips, ratio, up_steps, CORES, rows // kc, units), bf16),
            dma((2 + 2 * READS,)),
            dma((ratio, up_steps, CORES, chips)),
            dma((chips, ratio, up_steps, CORES)),
            dma((ratio, up_steps, CORES, chips)),
            dma((fs_count, kc)),
            dma((fs_count, kc, groups)),
            dma, dma,
            dma((col_chunks, k_pieces, chips)),
            dma((tp_count, col_chunks, k_pieces)),
            dma((tp_count, col_chunks, k_pieces, groups)),
            dma, dma,
            dma((fs_count, 2)),
            dma((fs_count,)),
            dma((tp_count, col_chunks, fs_count)),
            dma((fs_count, tp_count, col_chunks)),
        ],
        compiler_params=pltpu.CompilerParams(
            collective_id=0, has_side_effects=True, vmem_limit_bytes=40 * 1024 * 1024
        ),
    )(norm_gain.reshape(1, rows), up_weight, down_weight, prompt)
    any_space = pl.BlockSpec(memory_space=pl.ANY)
    return pl.pallas_call(
        write_out,
        out_shape=(
            jax.ShapeDtypeStruct(up_v.shape, bf16),
            jax.ShapeDtypeStruct(down_v.shape, bf16),
            jax.ShapeDtypeStruct(out_v.shape, bf16),
        ),
        in_specs=[vmem] * 3,
        out_specs=(any_space,) * 3,
        scratch_shapes=[dma((2 * PIECES + 1,))],
        compiler_params=pltpu.CompilerParams(vmem_limit_bytes=1024 * 1024),
        cost_estimate=pl.CostEstimate(flops=0, bytes_accessed=4 * depth * units * 2, transcendentals=0),
    )(up_v, down_v, out_v)


def solution(mesh):
    return jax.shard_map(
        functools.partial(per_device, mesh.shape["grp"]),
        mesh=mesh,
        in_specs=(P(("grp", "fs", "tp"), None), P("fs"), P("fs", "tp"), P("fs", "tp")),
        out_specs=(P("grp", "fs"), P("fs", "grp"), P(("grp", "fs", "tp"), None)),
        check_vma=False,
    )
```

```python
import functools

import jax
import jax.numpy as jnp
from jax import lax
from jax.experimental import pallas as pl
from jax.experimental.pallas import tpu as pltpu
from jax.sharding import PartitionSpec as P

epsilon = 1e-06
CORES = 2
PIECES = 4
UP_STEPS = 8
READS = 4
LANES = 128
K_PIECES = 4
WHOLE_PART = 0.75
AHEAD = 2
STAGE = (0.05, 0.45)
ARRIVAL = ((0.06, 0.52), (0.13, 0.55), (0.18, 0.78), (0.22, 1.02))
LAG_Y = 0.4
ROWS = (0.4, 0.9)
MESH = pl.DeviceIdType.MESH


def rank(origin, at, count):
    half = count // 2
    far = (origin < half) != (at < half)
    inner = abs(2 * origin - count + 1)
    if abs(2 * at - count + 1) > 1:
        return (far, -inner)
    return (-inner, not far)


def kernel(
    groups, fs_count, tp_count, up_steps, whole_cols, k_pieces,
    gain, up_w, down_w, prompt, up_v, down_v, out_v,
    gain_v, prompt_v, up_f, down_f, gain_col,
    ub, nb, nall, proj, hidden, pbuf, rbuf, stage,
    in_sem, up_send, stage_recv, z_send, up_recv, up_sib, upf_send, own_send, own_recv,
    dn_send, dn_recv, dn_sib, dnf_send, sib_send, sib_recv,
    n_send, n_recv, r_send, r_recv,
):
    y, z, t = lax.axis_index("grp"), lax.axis_index("fs"), lax.axis_index("tp")
    x, c = t // CORES, lax.rem(t, CORES)
    chips = tp_count // CORES
    ratio, rows, units = ub.shape
    chunk = rows // (up_steps * CORES * groups)
    width = down_w.shape[1]
    col_chunks = width // LANES
    k_rows = units // k_pieces
    tokens = prompt.shape[0]
    sibling = (y, z, x * CORES + 1 - c)
    t_src = z // ratio
    x_src, c_src = t_src // CORES, lax.rem(t_src, CORES)
    same_x = x == x_src

    up_part = rows // up_steps
    down_part = units // READS

    def up_read(i):
        at = pl.ds(i * up_part, up_part)
        return pltpu.make_async_copy(up_w.at[at, :], up_f.at[at, :], in_sem.at[2 + i])

    def down_read(i):
        at = pl.ds(i * down_part, down_part)
        return pltpu.make_async_copy(down_w.at[at, :], down_f.at[at, :], in_sem.at[2 + up_steps + i])

    gain_read = pltpu.make_async_copy(gain, gain_v, in_sem.at[0])
    prompt_read = pltpu.make_async_copy(prompt, prompt_v, in_sem.at[1])
    gain_read.start()
    up_read(0).start()
    prompt_read.start()
    for i in range(1, up_steps):
        up_read(i).start()
    for i in range(READS):
        down_read(i).start()

    barrier = pltpu.get_barrier_semaphore()
    peers = [sibling]
    peers += [(y, lax.rem(z + d, fs_count), x * CORES + cc) for d in range(1, fs_count) for cc in range(CORES)]
    peers += [(y, z, lax.rem(x + d, chips) * CORES + cc) for d in range(1, chips) for cc in range(CORES)]
    peers += [(lax.rem(y + g, groups), z, t) for g in range(1, groups)]
    for peer in peers:
        pl.semaphore_signal(barrier, inc=1, device_id=peer, device_id_type=MESH)

    gain_read.wait()
    gain_col[...] = jnp.broadcast_to(gain_v[...], (LANES, rows)).T
    step = min(16, up_part)

    def cast_up(n):
        up_read(n).wait()

        @pl.loop(0, up_part // step)
        def _(i):
            at = pl.ds(pl.multiple_of(n * up_part + i * step, step), step)
            factor = gain_col[at, :]
            for j in range(ratio):
                for b in range(units // LANES):
                    piece = up_f[at, j * units + b * LANES : j * units + (b + 1) * LANES]
                    ub[j, at, b * LANES : (b + 1) * LANES] = (factor * piece).astype(jnp.bfloat16)

    cast_up(0)
    pl.semaphore_wait(barrier, len(peers))

    def remote(src, dst, ssem, rsem, dev):
        return pltpu.make_async_remote_copy(
            src_ref=src, dst_ref=dst, send_sem=ssem, recv_sem=rsem, device_id=dev, device_id_type=MESH
        )

    def n_at(zr):
        return nall.at[pl.ds(pl.multiple_of(zr * tokens, tokens), tokens), :]

    def n_copy(zr, up, first):
        src = nb if first else n_at(zr)
        dev = (y, z + 1 if up else z - 1, t)
        return remote(src, n_at(zr), n_send.at[zr, int(up)], n_recv.at[zr], dev)

    def n_hop(h, act, wait):
        for up in (True, False):
            origin = z - h if up else z + h

            @pl.when(jnp.logical_and(origin >= 0, origin < fs_count))
            def _():
                if wait and h > 0:
                    remote(nb, n_at(origin), n_send.at[origin, int(up)], n_recv.at[origin], sibling).wait_recv()

                @pl.when(z < fs_count - 1 if up else z > 0)
                def _():
                    act(n_copy(origin, up, h == 0))

    def up_at(zr, k):
        return up_v.at[pl.ds(pl.multiple_of(zr * rows + k * chunk, chunk), chunk), :]

    def up_index(m, core, owner):
        return (m * CORES + core) * groups + owner

    def src_at(j, m, cd):
        k = up_index(m, cd, y)
        return ub.at[j, pl.ds(pl.multiple_of(k * chunk, chunk), chunk), :]

    def up_x(j, m, cd, dx):
        dev = (y, z, lax.rem(x + dx, chips) * CORES + c)
        sems = up_send.at[j, dx - 1], stage_recv.at[dx - 1, j, m]
        return remote(src_at(j, m, cd), stage.at[dx - 1, j, m, cd], *sems, dev)

    def up_x_own(j, m, cd, dx):
        dev = (y, z, lax.rem(x + dx, chips) * CORES + cd)
        k = up_index(m, cd, y)
        return remote(src_at(j, m, cd), up_at(z, k), up_send.at[j, dx - 1], up_recv.at[z, m, y], dev)

    def up_x_all(act, steps):
        for m in steps:
            for cd in range(CORES):
                for j in range(ratio):
                    mine = t * ratio + j == z
                    for dx in range(1, chips):
                        @pl.when(mine)
                        def _():
                            act(up_x_own(j, m, cd, dx))

                        @pl.when(jnp.logical_not(mine))
                        def _():
                            act(up_x(j, m, cd, dx))

    def up_z(j, m, cd, dx):
        xs = lax.rem(x + dx, chips)
        src = src_at(j, m, cd) if dx == 0 else stage.at[chips - dx - 1, j, m, cd]
        k = up_index(m, cd, y)
        dev = (y, (xs * CORES + c) * ratio + j, x * CORES + cd)
        return remote(src, up_at(z, k), z_send.at[j, dx], up_recv.at[z, m, y], dev)

    def away(j, dx, fn):
        pl.when((lax.rem(x + dx, chips) * CORES + c) * ratio + j != z)(fn)

    def go_z(m, j, dx):
        def go():
            if dx > 0:
                at = stage.at[chips - dx - 1, j, m]
                remote(at, at, up_send.at[j, 0], stage_recv.at[chips - dx - 1, j, m], sibling).wait_recv()
            for cd in range(CORES):
                up_z(j, m, cd, dx).start()

        away(j, dx, go)

    def z_own(m):
        for j in range(ratio):
            go_z(m, j, 0)

    def z_staged(m):
        for j in range(ratio):
            for dx in range(1, chips):
                go_z(m, j, dx)

    def sent(ref, sem):
        remote(ref, ref, sem, own_recv, sibling).wait_send()

    def landed(ref, sem):
        remote(ref, ref, own_send, sem, sibling).wait_recv()

    own_j = lax.rem(z, ratio)
    own_rows = pl.ds(pl.multiple_of(z * rows, rows), rows)
    my_cols = pl.ds(pl.multiple_of(t * width, width), width)

    def own_copy():
        return remote(ub.at[own_j], up_v.at[own_rows, :], own_send, own_recv, sibling)

    def sib_copy():
        return remote(down_v.at[:, my_cols], down_v.at[:, my_cols], sib_send, sib_recv, sibling)

    def cols_of(ts, i):
        return pl.ds(pl.multiple_of(ts * width + i * LANES, LANES), LANES)

    def dn_at(ts, i, k):
        return down_v.at[pl.ds(pl.multiple_of(k * k_rows, k_rows), k_rows), cols_of(ts, i)]

    def dn_col(ts, i):
        return down_v.at[:, cols_of(ts, i)]

    def dn_to(dx):
        return (y, z, lax.rem(x + dx, chips) * CORES + c)

    def dn_sends():
        for i in range(col_chunks):
            for n in range(1 if i < whole_cols else k_pieces // groups):
                for dx in range(1, chips):
                    if i < whole_cols:
                        at, sem = dn_col(t, i), dn_recv.at[dx - 1, i, 0]
                    else:
                        at, sem = dn_at(t, i, n * groups + y), dn_recv.at[dx - 1, i, n * groups + y]
                    remote(at, at, dn_send.at[int(i < whole_cols), dx - 1], sem, dn_to(dx)).start()

    start = lambda copy: copy.start()
    prompt_read.wait()
    widened = prompt_v[...].astype(jnp.float32)
    scale = lax.rsqrt(jnp.mean(widened * widened, axis=-1, keepdims=True) + epsilon)
    nb[...] = (widened * scale).astype(jnp.bfloat16)
    for m in range(up_steps):
        if m + 1 < up_steps and m > 0:
            cast_up(m + 1)
        up_x_all(start, (m,))
        if m < AHEAD:
            z_own(m)
        if m == 0:
            n_hop(0, start, False)
            if up_steps > 1:
                cast_up(1)

    @pl.when(t == t_src)
    def _():
        own_copy().start()

    down_step = min(64, down_part)
    for n in range(READS):
        down_read(n).wait()

        @pl.loop(0, down_part // down_step)
        def _(i):
            at = pl.ds(pl.multiple_of(n * down_part + i * down_step, down_step), down_step)
            down_v[at, my_cols] = down_f[at, :].astype(jnp.bfloat16)

    dn_sends()
    sib_copy().start()

    n_at(z)[...] = nb[...]

    @pl.when(t == t_src)
    def _():
        @pl.loop(0, rows // chunk)
        def _(i):
            part = pl.ds(pl.multiple_of(i * chunk, chunk), chunk)
            up_v[pl.ds(pl.multiple_of(z * rows + i * chunk, chunk), chunk), :] = ub[own_j, part, :]

    def up_y(zr, m, g):
        dev = (lax.rem(y + g, groups), z, t)
        at = up_at(zr, up_index(m, c, y))
        return remote(at, at, upf_send.at[zr, g], up_recv.at[zr, m, y], dev)

    def up_s(zr, m, owner):
        at = up_at(zr, up_index(m, c, owner))
        return remote(at, at, upf_send.at[zr, 0], up_sib.at[zr], sibling)

    def up_in(zr, m, owner):
        landed(up_at(zr, up_index(m, c, owner)), up_recv.at[zr, m, owner])

    def if_remote(d, fn):
        if d == 0:
            pl.when(jnp.logical_not(same_x))(fn)
        else:
            fn()

    def source(d):
        if d == 0 or fs_count > 8:
            return lax.rem(z + d, fs_count)
        found = 0
        for at in range(fs_count):
            order = sorted((o for o in range(fs_count) if o != at), key=lambda o: rank(o, at, fs_count))
            found = jnp.where(z == at, order[d - 1], found)
        return found

    def up_a(m, d):
        def go():
            zr = source(d)
            up_in(zr, m, y)
            for g in range(1, groups):
                up_y(zr, m, g).start()
            up_s(zr, m, y).start()

        if_remote(d, go)

    def up_b(m, d):
        def go():
            zr = source(d)
            for g in range(1, groups):
                owner = lax.rem(y + g, groups)
                up_in(zr, m, owner)
                up_s(zr, m, owner).start()

        if_remote(d, go)

    def up_c(d):
        if_remote(d, lambda: landed(up_v.at[pl.ds(0, rows // CORES), :], up_sib.at[source(d)]))

    def up_f(d):
        def go():
            zr = source(d)
            sent(up_v.at[pl.ds(0, rows // CORES), :], upf_send.at[zr, 0])
            for g in range(1, groups):
                sent(up_v.at[pl.ds(0, rows // (CORES * groups)), :], upf_send.at[zr, g])

        if_remote(d, go)

    def dn_src(dx):
        return lax.rem(x + dx, chips) * CORES + c

    def dn_whole(i, dx):
        at = dn_col(dn_src(dx), i)
        landed(at, dn_recv.at[chips - dx - 1, i, 0])
        remote(at, at, dnf_send.at[dx - 1, 0], dn_sib.at[dx - 1, i], sibling).start()

    def dn_piece(i, k, dx, forward):
        at, sem = dn_at(dn_src(dx), i, k), dn_recv.at[chips - dx - 1, i, k]
        landed(at, sem)
        if forward:
            for g in range(1, groups):
                remote(at, at, dnf_send.at[dx - 1, g], sem, (lax.rem(y + g, groups), z, t)).start()
        remote(at, at, dnf_send.at[dx - 1, 0], dn_sib.at[dx - 1, i], sibling).start()

    def dn_a(i, n, dx):
        dn_piece(i, n * groups + y, dx, True)

    def dn_b(i, n, dx):
        for g in range(1, groups):
            dn_piece(i, n * groups + lax.rem(y + g, groups), dx, False)

    part = functools.partial
    events = []
    for m in range(up_steps):
        share = m / max(1, up_steps - 1)
        when = STAGE[0] + (STAGE[1] - STAGE[0]) * share
        events.append((when, part(z_staged, m)))
        if m + AHEAD < up_steps:
            events.append((when + 0.001, part(z_own, m + AHEAD)))
        for d in range(fs_count):
            base, span = ARRIVAL[min(d, len(ARRIVAL) - 1)]
            when = max(base + (span - base) * share, STAGE[0] + (STAGE[1] - STAGE[0]) * share + 0.01) + 0.002 * d
            events.append((when, part(up_a, m, d)))
            events.append((when + LAG_Y, part(up_b, m, d)))
    for h in range(1, fs_count):
        when = ROWS[h - 1] if h <= len(ROWS) else 1.2 + h
        events.append((when, part(n_hop, h, start, True)))
    for i in range(whole_cols):
        for dx in range(1, chips):
            events.append((1.1, part(dn_whole, i, dx)))
    for _, event in sorted(events, key=lambda e: e[0]):
        event()

    for d in range(fs_count):
        up_c(d)

    @pl.when(jnp.logical_and(same_x, t != t_src))
    def _():
        own_copy().wait_recv()

    depth = prompt.shape[1]
    kb = 256
    nb_tile = min(units, 1024)

    split = range(whole_cols, col_chunks)
    rest = [part(dn_a, i, n, dx) for i in split for n in range(k_pieces // groups) for dx in range(1, chips)]
    pieces = depth // kb
    done = 0
    for i in range(pieces):
        for j in range(units // nb_tile):
            col = pl.ds(j * nb_tile, nb_tile)
            term = jnp.dot(
                nall[:, i * kb : (i + 1) * kb],
                up_v[i * kb : (i + 1) * kb, col],
                preferred_element_type=jnp.float32,
            )
            if i == 0:
                proj[:, col] = term
            else:
                proj[:, col] += term
        upto = len(rest) * (i + 1) // (2 * pieces)
        for fn in rest[done:upto]:
            fn()
        done = upto

    positive = jnp.maximum(proj[...], 0.0)
    hidden[...] = (positive * positive).astype(jnp.bfloat16)

    def r_copy(ts, i, wide, d):
        zt = lax.rem(z + d, fs_count)
        cols = pl.ds(pl.multiple_of(ts * width + i * LANES, LANES), wide)
        return remote(pbuf.at[zt, :, cols], rbuf.at[z, :, cols], r_send.at[d], r_recv.at[z], (y, zt, t))

    def block(ts, i, wide):
        cols = pl.ds(pl.multiple_of(ts * width + i * LANES, LANES), wide)
        part = jnp.dot(hidden[...], down_v[:, cols], preferred_element_type=jnp.float32).astype(jnp.bfloat16)
        pbuf[:, :, cols] = part.reshape(fs_count, tokens, wide)

    blocks = [(t, 0, width), (x * CORES + 1 - c, 0, width)]
    for i in range(col_chunks):
        for dx in range(1, chips):
            blocks += [(dn_src(dx), i, LANES), (lax.rem(x + dx, chips) * CORES + 1 - c, i, LANES)]

    def send_block(ts, i, wide):
        for d in range(1, fs_count):
            r_copy(ts, i, wide, d).start()

    last = None
    for index, (ts, i, wide) in enumerate(blocks):
        if index == 1:
            sib_copy().wait_recv()
        if index >= CORES:
            dx = 1 + (index - CORES) // CORES % (chips - 1)
            if (index - CORES) % CORES == 0 and i >= whole_cols:
                for n in range(k_pieces // groups):
                    dn_b(i, n, dx)
            if (index - CORES) % CORES == 1:
                landed(dn_col(ts, i), dn_sib.at[dx - 1, i])
        block(ts, i, wide)
        if index < CORES:
            upto = len(rest) if index == CORES - 1 else (done + len(rest)) // 2
            for fn in rest[done:upto]:
                fn()
            done = upto
        if last is not None:
            send_block(*last)
        last = (ts, i, wide)
    send_block(*last)

    total = pbuf[z].astype(jnp.float32)

    @pl.loop(1, fs_count)
    def _(d):
        zr = lax.rem(z + d, fs_count)
        remote(pbuf.at[zr], rbuf.at[zr], r_send.at[d], r_recv.at[zr], (y, zr, t)).wait()

    for d in range(1, fs_count):
        total += rbuf[lax.rem(z + d, fs_count)].astype(jnp.float32)
    out_v[...] = total.astype(jnp.bfloat16)

    for d in range(fs_count):
        up_f(d)
    for dx in range(1, chips):
        sent(down_v.at[:, pl.ds(0, width)], dnf_send.at[dx - 1, 0])
        if whole_cols > 0:
            sent(down_v.at[:, pl.ds(0, whole_cols * LANES)], dn_send.at[1, dx - 1])
        if whole_cols < col_chunks:
            half = down_v.at[pl.ds(0, units // groups), pl.ds(0, (col_chunks - whole_cols) * LANES)]
            sent(half, dn_send.at[0, dx - 1])
            for g in range(1, groups):
                sent(half, dnf_send.at[dx - 1, g])
    for j in range(ratio):
        half = up_v.at[pl.ds(0, rows // groups), :]
        for dx in range(1, chips):
            sent(half, up_send.at[j, dx - 1])
        for dx in range(chips):
            away(j, dx, functools.partial(sent, half, z_send.at[j, dx]))
    sib_copy().wait_send()

    @pl.when(t == t_src)
    def _():
        own_copy().wait_send()

    for h in range(fs_count):
        n_hop(h, lambda copy: copy.wait_send(), False)


def write_out(up_v, down_v, out_v, up_out, down_out, mlp_out, sems):
    copies = [pltpu.make_async_copy(out_v, mlp_out, sems.at[2 * PIECES])]
    for n, (src, dst) in enumerate(((up_v, up_out), (down_v, down_out))):
        step = src.shape[0] // PIECES
        for i in range(PIECES):
            part = pl.ds(i * step, step)
            copies.append(pltpu.make_async_copy(src.at[part, :], dst.at[part, :], sems.at[n * PIECES + i]))
    for copy in copies:
        copy.start()
    for copy in copies:
        copy.wait()


def per_device(groups, prompt, norm_gain, up_weight, down_weight):
    tp_count, fs_count = lax.axis_size("tp"), lax.axis_size("fs")
    rows, wide = up_weight.shape
    units, width = down_weight.shape
    tokens, depth = prompt.shape
    ratio = wide // units
    up_steps = max(1, min(UP_STEPS, rows // (CORES * groups * 16)))
    col_chunks = width // LANES
    whole_cols = int(col_chunks * WHOLE_PART)
    chips = tp_count // CORES
    kc = up_steps * CORES * groups
    k_pieces = K_PIECES
    f32, bf16 = jnp.float32, jnp.bfloat16
    dma = pltpu.SemaphoreType.DMA
    vmem = pl.BlockSpec(memory_space=pltpu.VMEM)
    hbm = pl.BlockSpec(memory_space=pltpu.HBM)
    up_v, down_v, out_v = pl.pallas_call(
        functools.partial(kernel, groups, fs_count, tp_count, up_steps, whole_cols, k_pieces),
        out_shape=(
            pltpu.VMEM((depth, units), bf16),
            pltpu.VMEM((units, depth), bf16),
            pltpu.VMEM((tokens, depth), bf16),
        ),
        in_specs=[hbm] * 4,
        out_specs=(vmem,) * 3,
        scratch_shapes=[
            pltpu.VMEM((1, rows), f32),
            pltpu.VMEM((tokens, depth), bf16),
            pltpu.VMEM((rows, wide), f32),
            pltpu.VMEM((units, width), f32),
            pltpu.VMEM((rows, LANES), f32),
            pltpu.VMEM((ratio, rows, units), bf16),
            pltpu.VMEM((tokens, depth), bf16),
            pltpu.VMEM((fs_count * tokens, depth), bf16),
            pltpu.VMEM((fs_count * tokens, units), f32),
            pltpu.VMEM((fs_count * tokens, units), bf16),
            pltpu.VMEM((fs_count, tokens, depth), bf16),
            pltpu.VMEM((fs_count, tokens, depth), bf16),
            pltpu.VMEM((chips - 1, ratio, up_steps, CORES, rows // kc, units), bf16),
            dma((2 + up_steps + READS,)),
            dma((ratio, chips - 1)),
            dma((chips - 1, ratio, up_steps)),
            dma((ratio, chips)),
            dma((fs_count, up_steps, groups)),
            dma((fs_count,)),
            dma((fs_count, groups)),
            dma, dma,
            dma((2, chips - 1)),
            dma((chips - 1, col_chunks, k_pieces)),
            dma((chips - 1, col_chunks)),
            dma((chips - 1, groups)),
            dma, dma,
            dma((fs_count, 2)),
            dma((fs_count,)),
            dma((fs_count,)),
            dma((fs_count,)),
        ],
        compiler_params=pltpu.CompilerParams(
            collective_id=0, has_side_effects=True, vmem_limit_bytes=40 * 1024 * 1024
        ),
    )(norm_gain.reshape(1, rows), up_weight, down_weight, prompt)
    any_space = pl.BlockSpec(memory_space=pl.ANY)
    return pl.pallas_call(
        write_out,
        out_shape=(
            jax.ShapeDtypeStruct(up_v.shape, bf16),
            jax.ShapeDtypeStruct(down_v.shape, bf16),
            jax.ShapeDtypeStruct(out_v.shape, bf16),
        ),
        in_specs=[vmem] * 3,
        out_specs=(any_space,) * 3,
        scratch_shapes=[dma((2 * PIECES + 1,))],
        compiler_params=pltpu.CompilerParams(vmem_limit_bytes=1024 * 1024),
        cost_estimate=pl.CostEstimate(flops=0, bytes_accessed=4 * depth * units * 2, transcendentals=0),
    )(up_v, down_v, out_v)


def solution(mesh):
    return jax.shard_map(
        functools.partial(per_device, mesh.shape["grp"]),
        mesh=mesh,
        in_specs=(P(("grp", "fs", "tp"), None), P("fs"), P("fs", "tp"), P("fs", "tp")),
        out_specs=(P("grp", "fs"), P("fs", "grp"), P(("grp", "fs", "tp"), None)),
        check_vma=False,
    )
```

```python
import functools

import jax
import jax.numpy as jnp
from jax import lax
from jax.experimental import pallas as pl
from jax.experimental.pallas import tpu as pltpu
from jax.sharding import PartitionSpec as P

epsilon = 1e-06
CORES = 2
PIECES = 4
UP_STEPS = 8
READS = 4
LANES = 128
K_PIECES = 4
WHOLE_PART = 0.75
AHEAD = 2
FEED = 0.012
DOWN_TURN = 1.03
DOWN_CAST = 0.13
STAGE = (0.05, 0.45)
ARRIVAL = ((0.06, 0.52), (0.13, 0.55), (0.18, 0.78), (0.22, 1.02))
LAG_Y = 0.4
ROWS = (0.55, 1.0)
MESH = pl.DeviceIdType.MESH


def rank(origin, at, count):
    half = count // 2
    far = (origin < half) != (at < half)
    inner = abs(2 * origin - count + 1)
    if abs(2 * at - count + 1) > 1:
        return (far, -inner)
    return (-inner, not far)


def kernel(
    groups, fs_count, tp_count, up_steps, whole_cols, k_pieces,
    gain, up_w, down_w, prompt, up_v, down_v, out_v,
    gain_v, prompt_v, up_f, down_f, gain_col,
    ub, nb, nall, proj, hidden, pbuf, rbuf, stage,
    in_sem, up_send, stage_recv, z_send, up_recv, up_sib, upf_send, own_send, own_recv,
    dn_send, dn_recv, dn_sib, dnf_send, sib_send, sib_recv,
    n_send, n_recv, r_send, r_recv,
):
    y, z, t = lax.axis_index("grp"), lax.axis_index("fs"), lax.axis_index("tp")
    x, c = t // CORES, lax.rem(t, CORES)
    chips = tp_count // CORES
    ratio, rows, units = ub.shape
    chunk = rows // (up_steps * CORES * groups)
    width = down_w.shape[1]
    col_chunks = width // LANES
    k_rows = units // k_pieces
    lead = whole_cols - whole_cols // 2 if col_chunks < 3 else max(0, whole_cols - 1)
    split = range(lead, lead + col_chunks - whole_cols)

    def whole(i):
        return i not in split

    tokens = prompt.shape[0]
    sibling = (y, z, x * CORES + 1 - c)
    t_src = z // ratio
    x_src, c_src = t_src // CORES, lax.rem(t_src, CORES)
    same_x = x == x_src

    up_part = rows // up_steps
    down_part = units // READS

    def up_read(i):
        at = pl.ds(i * up_part, up_part)
        return pltpu.make_async_copy(up_w.at[at, :], up_f.at[at, :], in_sem.at[2 + i])

    def down_read(i):
        at = pl.ds(i * down_part, down_part)
        return pltpu.make_async_copy(down_w.at[at, :], down_f.at[at, :], in_sem.at[2 + up_steps + i])

    gain_read = pltpu.make_async_copy(gain, gain_v, in_sem.at[0])
    prompt_read = pltpu.make_async_copy(prompt, prompt_v, in_sem.at[1])
    gain_read.start()
    up_read(0).start()
    prompt_read.start()
    for i in range(1, up_steps):
        up_read(i).start()
    for i in range(READS):
        down_read(i).start()

    barrier = pltpu.get_barrier_semaphore()
    peers = [sibling]
    peers += [(y, lax.rem(z + d, fs_count), x * CORES + cc) for d in range(1, fs_count) for cc in range(CORES)]
    peers += [(y, z, lax.rem(x + d, chips) * CORES + cc) for d in range(1, chips) for cc in range(CORES)]
    peers += [(lax.rem(y + g, groups), z, t) for g in range(1, groups)]
    for peer in peers:
        pl.semaphore_signal(barrier, inc=1, device_id=peer, device_id_type=MESH)

    gain_read.wait()
    gain_col[...] = jnp.broadcast_to(gain_v[...], (LANES, rows)).T
    step = min(16, up_part)

    def cast_up(n):
        up_read(n).wait()

        @pl.loop(0, up_part // step)
        def _(i):
            at = pl.ds(pl.multiple_of(n * up_part + i * step, step), step)
            factor = gain_col[at, :]
            for j in range(ratio):
                for b in range(units // LANES):
                    piece = up_f[at, j * units + b * LANES : j * units + (b + 1) * LANES]
                    ub[j, at, b * LANES : (b + 1) * LANES] = (factor * piece).astype(jnp.bfloat16)

    cast_up(0)
    pl.semaphore_wait(barrier, len(peers))

    def remote(src, dst, ssem, rsem, dev):
        return pltpu.make_async_remote_copy(
            src_ref=src, dst_ref=dst, send_sem=ssem, recv_sem=rsem, device_id=dev, device_id_type=MESH
        )

    def n_at(zr):
        return nall.at[pl.ds(pl.multiple_of(zr * tokens, tokens), tokens), :]

    def n_copy(zr, up, first):
        src = nb if first else n_at(zr)
        dev = (y, z + 1 if up else z - 1, t)
        return remote(src, n_at(zr), n_send.at[zr, int(up)], n_recv.at[zr], dev)

    def n_hop(h, act, wait):
        for up in (True, False):
            origin = z - h if up else z + h

            @pl.when(jnp.logical_and(origin >= 0, origin < fs_count))
            def _():
                if wait and h > 0:
                    remote(nb, n_at(origin), n_send.at[origin, int(up)], n_recv.at[origin], sibling).wait_recv()

                @pl.when(z < fs_count - 1 if up else z > 0)
                def _():
                    act(n_copy(origin, up, h == 0))

    def up_at(zr, k):
        return up_v.at[pl.ds(pl.multiple_of(zr * rows + k * chunk, chunk), chunk), :]

    def up_index(m, core, owner):
        return (m * CORES + core) * groups + owner

    def src_at(j, m, cd):
        k = up_index(m, cd, y)
        return ub.at[j, pl.ds(pl.multiple_of(k * chunk, chunk), chunk), :]

    def up_x(j, m, cd, dx):
        dev = (y, z, lax.rem(x + dx, chips) * CORES + c)
        sems = up_send.at[j, dx - 1], stage_recv.at[dx - 1, j, m]
        return remote(src_at(j, m, cd), stage.at[dx - 1, j, m, cd], *sems, dev)

    def up_x_own(j, m, cd, dx):
        dev = (y, z, lax.rem(x + dx, chips) * CORES + cd)
        k = up_index(m, cd, y)
        return remote(src_at(j, m, cd), up_at(z, k), up_send.at[j, dx - 1], up_recv.at[z, m, y], dev)

    def up_x_all(act, steps):
        for m in steps:
            for cd in range(CORES):
                for j in range(ratio):
                    mine = t * ratio + j == z
                    for dx in range(1, chips):
                        @pl.when(mine)
                        def _():
                            act(up_x_own(j, m, cd, dx))

                        @pl.when(jnp.logical_not(mine))
                        def _():
                            act(up_x(j, m, cd, dx))

    def up_z(j, m, cd, dx):
        xs = lax.rem(x + dx, chips)
        src = src_at(j, m, cd) if dx == 0 else stage.at[chips - dx - 1, j, m, cd]
        k = up_index(m, cd, y)
        dev = (y, (xs * CORES + c) * ratio + j, x * CORES + cd)
        return remote(src, up_at(z, k), z_send.at[j, dx], up_recv.at[z, m, y], dev)

    def away(j, dx, fn):
        pl.when((lax.rem(x + dx, chips) * CORES + c) * ratio + j != z)(fn)

    def go_z(m, j, dx):
        def go():
            if dx > 0:
                at = stage.at[chips - dx - 1, j, m]
                remote(at, at, up_send.at[j, 0], stage_recv.at[chips - dx - 1, j, m], sibling).wait_recv()
            for cd in range(CORES):
                up_z(j, m, cd, dx).start()

        away(j, dx, go)

    def z_own(m):
        for j in range(ratio):
            go_z(m, j, 0)

    def z_staged(m):
        for j in range(ratio):
            for dx in range(1, chips):
                go_z(m, j, dx)

    def sent(ref, sem):
        remote(ref, ref, sem, own_recv, sibling).wait_send()

    def landed(ref, sem):
        remote(ref, ref, own_send, sem, sibling).wait_recv()

    own_j = lax.rem(z, ratio)
    own_rows = pl.ds(pl.multiple_of(z * rows, rows), rows)
    my_cols = pl.ds(pl.multiple_of(t * width, width), width)

    def own_copy():
        return remote(ub.at[own_j], up_v.at[own_rows, :], own_send, own_recv, sibling)

    def sib_copy():
        return remote(down_v.at[:, my_cols], down_v.at[:, my_cols], sib_send, sib_recv, sibling)

    def cols_of(ts, i):
        return pl.ds(pl.multiple_of(ts * width + i * LANES, LANES), LANES)

    def dn_at(ts, i, k):
        return down_v.at[pl.ds(pl.multiple_of(k * k_rows, k_rows), k_rows), cols_of(ts, i)]

    def dn_col(ts, i):
        return down_v.at[:, cols_of(ts, i)]

    def dn_to(dx):
        return (y, z, lax.rem(x + dx, chips) * CORES + c)

    def dn_sends():
        for i in range(col_chunks):
            for n in range(1 if whole(i) else k_pieces // groups):
                for dx in range(1, chips):
                    if whole(i):
                        at, sem = dn_col(t, i), dn_recv.at[dx - 1, i, 0]
                    else:
                        at, sem = dn_at(t, i, n * groups + y), dn_recv.at[dx - 1, i, n * groups + y]
                    remote(at, at, dn_send.at[int(whole(i)), dx - 1], sem, dn_to(dx)).start()

    start = lambda copy: copy.start()
    prompt_read.wait()
    widened = prompt_v[...].astype(jnp.float32)
    scale = lax.rsqrt(jnp.mean(widened * widened, axis=-1, keepdims=True) + epsilon)
    nb[...] = (widened * scale).astype(jnp.bfloat16)
    def feed(m):
        if m + 1 < up_steps:
            cast_up(m + 1)
        up_x_all(start, (m,))
        if m < AHEAD:
            z_own(m)

    up_x_all(start, (0,))
    z_own(0)
    n_hop(0, start, False)
    if up_steps > 1:
        cast_up(1)

    down_step = min(64, down_part)

    def cast_down(n):
        down_read(n).wait()

        @pl.loop(0, down_part // down_step)
        def _(i):
            at = pl.ds(pl.multiple_of(n * down_part + i * down_step, down_step), down_step)
            down_v[at, my_cols] = down_f[at, :].astype(jnp.bfloat16)

    def start_down():
        dn_sends()
        sib_copy().start()

    def keep_own():
        n_at(z)[...] = nb[...]

        @pl.when(t == t_src)
        def _():
            own_copy().start()

            @pl.loop(0, rows // chunk)
            def _(i):
                part = pl.ds(pl.multiple_of(i * chunk, chunk), chunk)
                up_v[pl.ds(pl.multiple_of(z * rows + i * chunk, chunk), chunk), :] = ub[own_j, part, :]

    def up_y(zr, m, g):
        dev = (lax.rem(y + g, groups), z, t)
        at = up_at(zr, up_index(m, c, y))
        return remote(at, at, upf_send.at[zr, g], up_recv.at[zr, m, y], dev)

    def up_s(zr, m, owner):
        at = up_at(zr, up_index(m, c, owner))
        return remote(at, at, upf_send.at[zr, 0], up_sib.at[zr], sibling)

    def up_in(zr, m, owner):
        landed(up_at(zr, up_index(m, c, owner)), up_recv.at[zr, m, owner])

    def if_remote(d, fn):
        if d == 0:
            pl.when(jnp.logical_not(same_x))(fn)
        else:
            fn()

    def source(d):
        if d == 0 or fs_count > 8:
            return lax.rem(z + d, fs_count)
        found = 0
        for at in range(fs_count):
            order = sorted((o for o in range(fs_count) if o != at), key=lambda o: rank(o, at, fs_count))
            found = jnp.where(z == at, order[d - 1], found)
        return found

    def up_a(m, d):
        def go():
            zr = source(d)
            up_in(zr, m, y)
            for g in range(1, groups):
                up_y(zr, m, g).start()
            up_s(zr, m, y).start()

        if_remote(d, go)

    def up_b(m, d):
        def go():
            zr = source(d)
            for g in range(1, groups):
                owner = lax.rem(y + g, groups)
                up_in(zr, m, owner)
                up_s(zr, m, owner).start()

        if_remote(d, go)

    def up_c(d):
        if_remote(d, lambda: landed(up_v.at[pl.ds(0, rows // CORES), :], up_sib.at[source(d)]))

    def up_done(d):
        def go():
            zr = source(d)
            sent(up_v.at[pl.ds(0, rows // CORES), :], upf_send.at[zr, 0])
            for g in range(1, groups):
                sent(up_v.at[pl.ds(0, rows // (CORES * groups)), :], upf_send.at[zr, g])

        if_remote(d, go)

    def dn_src(dx):
        return lax.rem(x + dx, chips) * CORES + c

    def dn_whole(i, dx):
        at = dn_col(dn_src(dx), i)
        landed(at, dn_recv.at[chips - dx - 1, i, 0])
        remote(at, at, dnf_send.at[dx - 1, 0], dn_sib.at[dx - 1, i], sibling).start()

    def dn_piece(i, k, dx, forward):
        at, sem = dn_at(dn_src(dx), i, k), dn_recv.at[chips - dx - 1, i, k]
        landed(at, sem)
        if forward:
            for g in range(1, groups):
                remote(at, at, dnf_send.at[dx - 1, g], sem, (lax.rem(y + g, groups), z, t)).start()
        remote(at, at, dnf_send.at[dx - 1, 0], dn_sib.at[dx - 1, i], sibling).start()

    def dn_a(i, n, dx):
        dn_piece(i, n * groups + y, dx, True)

    def dn_b(i, n, dx):
        for g in range(1, groups):
            dn_piece(i, n * groups + lax.rem(y + g, groups), dx, False)

    part = functools.partial
    events, queued = [], []
    for m in range(1, up_steps):
        events.append((FEED * m, part(feed, m)))
    for n in range(READS):
        events.append((DOWN_CAST + 0.03 * n, part(cast_down, n)))
    events.append((DOWN_CAST + 0.03 * READS, start_down))
    events.append((DOWN_CAST + 0.03 * READS + 0.05, keep_own))
    for m in range(up_steps):
        share = m / max(1, up_steps - 1)
        when = STAGE[0] + (STAGE[1] - STAGE[0]) * share
        events.append((when, part(z_staged, m)))
        if m + AHEAD < up_steps:
            events.append((when + 0.001, part(z_own, m + AHEAD)))
        for d in range(fs_count):
            base, span = ARRIVAL[min(d, len(ARRIVAL) - 1)]
            when = max(base + (span - base) * share, STAGE[0] + (STAGE[1] - STAGE[0]) * share + 0.01) + 0.002 * d
            events.append((when, part(up_a, m, d)))
            events.append((when + LAG_Y, part(up_b, m, d)))
    for h in range(1, fs_count):
        when = ROWS[h - 1] if h <= len(ROWS) else 1.2 + h
        events.append((when, part(n_hop, h, start, True)))
    for i in range(lead):
        for dx in range(1, chips):
            events.append((1.1, part(dn_whole, i, dx)))
    for i in split:
        for n in range(k_pieces // groups):
            for dx in range(1, chips):
                events.append((DOWN_TURN + 0.001 * i, part(dn_a, i, n, dx)))
    for _, event in sorted(events, key=lambda e: e[0]):
        event()

    for d in range(fs_count):
        up_c(d)

    @pl.when(jnp.logical_and(same_x, t != t_src))
    def _():
        own_copy().wait_recv()

    depth = prompt.shape[1]
    kb = 256
    nb_tile = min(units, 1024)

    pieces = depth // kb
    for i in range(pieces):
        for j in range(units // nb_tile):
            col = pl.ds(j * nb_tile, nb_tile)
            term = jnp.dot(
                nall[:, i * kb : (i + 1) * kb],
                up_v[i * kb : (i + 1) * kb, col],
                preferred_element_type=jnp.float32,
            )
            if i == 0:
                proj[:, col] = term
            else:
                proj[:, col] += term

    positive = jnp.maximum(proj[...], 0.0)
    hidden[...] = (positive * positive).astype(jnp.bfloat16)

    def r_copy(ts, i, wide, d):
        zt = lax.rem(z + d, fs_count)
        cols = pl.ds(pl.multiple_of(ts * width + i * LANES, LANES), wide)
        return remote(pbuf.at[zt, :, cols], rbuf.at[z, :, cols], r_send.at[d], r_recv.at[z], (y, zt, t))

    def block(ts, i, wide):
        cols = pl.ds(pl.multiple_of(ts * width + i * LANES, LANES), wide)
        part = jnp.dot(hidden[...], down_v[:, cols], preferred_element_type=jnp.float32).astype(jnp.bfloat16)
        pbuf[:, :, cols] = part.reshape(fs_count, tokens, wide)

    blocks = [(t, 0, width), (x * CORES + 1 - c, 0, width)]
    for i in range(col_chunks):
        for dx in range(1, chips):
            blocks += [(dn_src(dx), i, LANES), (lax.rem(x + dx, chips) * CORES + 1 - c, i, LANES)]

    def send_block(ts, i, wide):
        for d in range(1, fs_count):
            r_copy(ts, i, wide, d).start()

    last = None
    for index, (ts, i, wide) in enumerate(blocks):
        if index == 1:
            sib_copy().wait_recv()
        if index >= CORES:
            dx = 1 + (index - CORES) // CORES % (chips - 1)
            if (index - CORES) % CORES == 0 and whole(i) and i >= lead:
                dn_whole(i, dx)
            if (index - CORES) % CORES == 0 and not whole(i):
                for n in range(k_pieces // groups):
                    dn_b(i, n, dx)
            if (index - CORES) % CORES == 1:
                landed(dn_col(ts, i), dn_sib.at[dx - 1, i])
        block(ts, i, wide)
        if last is not None:
            send_block(*last)
        last = (ts, i, wide)
    send_block(*last)

    total = pbuf[z].astype(jnp.float32)

    @pl.loop(1, fs_count)
    def _(d):
        zr = lax.rem(z + d, fs_count)
        remote(pbuf.at[zr], rbuf.at[zr], r_send.at[d], r_recv.at[zr], (y, zr, t)).wait()

    for d in range(1, fs_count):
        total += rbuf[lax.rem(z + d, fs_count)].astype(jnp.float32)
    out_v[...] = total.astype(jnp.bfloat16)

    for d in range(fs_count):
        up_done(d)
    for dx in range(1, chips):
        sent(down_v.at[:, pl.ds(0, width)], dnf_send.at[dx - 1, 0])
        if whole_cols > 0:
            sent(down_v.at[:, pl.ds(0, whole_cols * LANES)], dn_send.at[1, dx - 1])
        if whole_cols < col_chunks:
            half = down_v.at[pl.ds(0, units // groups), pl.ds(0, (col_chunks - whole_cols) * LANES)]
            sent(half, dn_send.at[0, dx - 1])
            for g in range(1, groups):
                sent(half, dnf_send.at[dx - 1, g])
    for j in range(ratio):
        half = up_v.at[pl.ds(0, rows // groups), :]
        for dx in range(1, chips):
            sent(half, up_send.at[j, dx - 1])
        for dx in range(chips):
            away(j, dx, functools.partial(sent, half, z_send.at[j, dx]))
    sib_copy().wait_send()

    @pl.when(t == t_src)
    def _():
        own_copy().wait_send()

    for h in range(fs_count):
        n_hop(h, lambda copy: copy.wait_send(), False)


def write_out(up_v, down_v, out_v, up_out, down_out, mlp_out, sems):
    copies = [pltpu.make_async_copy(out_v, mlp_out, sems.at[2 * PIECES])]
    for n, (src, dst) in enumerate(((up_v, up_out), (down_v, down_out))):
        step = src.shape[0] // PIECES
        for i in range(PIECES):
            part = pl.ds(i * step, step)
            copies.append(pltpu.make_async_copy(src.at[part, :], dst.at[part, :], sems.at[n * PIECES + i]))
    for copy in copies:
        copy.start()
    for copy in copies:
        copy.wait()


def per_device(groups, prompt, norm_gain, up_weight, down_weight):
    tp_count, fs_count = lax.axis_size("tp"), lax.axis_size("fs")
    rows, wide = up_weight.shape
    units, width = down_weight.shape
    tokens, depth = prompt.shape
    ratio = wide // units
    up_steps = max(1, min(UP_STEPS, rows // (CORES * groups * 16)))
    col_chunks = width // LANES
    whole_cols = int(col_chunks * WHOLE_PART)
    chips = tp_count // CORES
    kc = up_steps * CORES * groups
    k_pieces = K_PIECES
    f32, bf16 = jnp.float32, jnp.bfloat16
    dma = pltpu.SemaphoreType.DMA
    vmem = pl.BlockSpec(memory_space=pltpu.VMEM)
    hbm = pl.BlockSpec(memory_space=pltpu.HBM)
    up_v, down_v, out_v = pl.pallas_call(
        functools.partial(kernel, groups, fs_count, tp_count, up_steps, whole_cols, k_pieces),
        out_shape=(
            pltpu.VMEM((depth, units), bf16),
            pltpu.VMEM((units, depth), bf16),
            pltpu.VMEM((tokens, depth), bf16),
        ),
        in_specs=[hbm] * 4,
        out_specs=(vmem,) * 3,
        scratch_shapes=[
            pltpu.VMEM((1, rows), f32),
            pltpu.VMEM((tokens, depth), bf16),
            pltpu.VMEM((rows, wide), f32),
            pltpu.VMEM((units, width), f32),
            pltpu.VMEM((rows, LANES), f32),
            pltpu.VMEM((ratio, rows, units), bf16),
            pltpu.VMEM((tokens, depth), bf16),
            pltpu.VMEM((fs_count * tokens, depth), bf16),
            pltpu.VMEM((fs_count * tokens, units), f32),
            pltpu.VMEM((fs_count * tokens, units), bf16),
            pltpu.VMEM((fs_count, tokens, depth), bf16),
            pltpu.VMEM((fs_count, tokens, depth), bf16),
            pltpu.VMEM((chips - 1, ratio, up_steps, CORES, rows // kc, units), bf16),
            dma((2 + up_steps + READS,)),
            dma((ratio, chips - 1)),
            dma((chips - 1, ratio, up_steps)),
            dma((ratio, chips)),
            dma((fs_count, up_steps, groups)),
            dma((fs_count,)),
            dma((fs_count, groups)),
            dma, dma,
            dma((2, chips - 1)),
            dma((chips - 1, col_chunks, k_pieces)),
            dma((chips - 1, col_chunks)),
            dma((chips - 1, groups)),
            dma, dma,
            dma((fs_count, 2)),
            dma((fs_count,)),
            dma((fs_count,)),
            dma((fs_count,)),
        ],
        compiler_params=pltpu.CompilerParams(
            collective_id=0, has_side_effects=True, vmem_limit_bytes=40 * 1024 * 1024
        ),
    )(norm_gain.reshape(1, rows), up_weight, down_weight, prompt)
    any_space = pl.BlockSpec(memory_space=pl.ANY)
    return pl.pallas_call(
        write_out,
        out_shape=(
            jax.ShapeDtypeStruct(up_v.shape, bf16),
            jax.ShapeDtypeStruct(down_v.shape, bf16),
            jax.ShapeDtypeStruct(out_v.shape, bf16),
        ),
        in_specs=[vmem] * 3,
        out_specs=(any_space,) * 3,
        scratch_shapes=[dma((2 * PIECES + 1,))],
        compiler_params=pltpu.CompilerParams(vmem_limit_bytes=1024 * 1024),
        cost_estimate=pl.CostEstimate(flops=0, bytes_accessed=4 * depth * units * 2, transcendentals=0),
    )(up_v, down_v, out_v)


def solution(mesh):
    return jax.shard_map(
        functools.partial(per_device, mesh.shape["grp"]),
        mesh=mesh,
        in_specs=(P(("grp", "fs", "tp"), None), P("fs"), P("fs", "tp"), P("fs", "tp")),
        out_specs=(P("grp", "fs"), P("fs", "grp"), P(("grp", "fs", "tp"), None)),
        check_vma=False,
    )
```

```python
import functools

import jax
import jax.numpy as jnp
from jax import lax
from jax.experimental import pallas as pl
from jax.experimental.pallas import tpu as pltpu
from jax.sharding import PartitionSpec as P

epsilon = 1e-06
CORES = 2
PIECES = 4
UP_STEPS = 8
READS = 4
LANES = 128
K_PIECES = 4
WHOLE_PART = 0.75
AHEAD = 2
FEED = 0.012
DOWN_TURN = 1.03
DOWN_CAST = 0.13
STAGE = (0.05, 0.45)
ARRIVAL = ((0.06, 0.52), (0.13, 0.55), (0.18, 0.78), (0.22, 1.02))
LAG_Y = 0.4
ROWS = (0.75, 1.03)
MESH = pl.DeviceIdType.MESH


def rank(origin, at, count):
    half = count // 2
    far = (origin < half) != (at < half)
    inner = abs(2 * origin - count + 1)
    if abs(2 * at - count + 1) > 1:
        return (far, -inner)
    return (-inner, not far)


def kernel(
    groups, fs_count, tp_count, up_steps, whole_cols, k_pieces,
    gain, up_w, down_w, prompt, up_v, down_v, out_v,
    gain_v, prompt_v, up_f, down_f, gain_col,
    ub, nb, nall, proj, hidden, pbuf, rbuf, stage,
    in_sem, up_send, stage_recv, z_send, up_recv, up_sib, upf_send, own_send, own_recv,
    dn_send, dn_recv, dn_sib, dnf_send, sib_send, sib_recv,
    n_send, n_recv, r_send, r_recv,
):
    y, z, t = lax.axis_index("grp"), lax.axis_index("fs"), lax.axis_index("tp")
    x, c = t // CORES, lax.rem(t, CORES)
    chips = tp_count // CORES
    ratio, rows, units = ub.shape
    chunk = rows // (up_steps * CORES * groups)
    width = down_w.shape[1]
    col_chunks = width // LANES
    k_rows = units // k_pieces
    lead = whole_cols - whole_cols // 2 if col_chunks < 3 else max(0, whole_cols - 1)
    split = range(lead, lead + col_chunks - whole_cols)

    def whole(i):
        return i not in split

    tokens = prompt.shape[0]
    sibling = (y, z, x * CORES + 1 - c)
    t_src = z // ratio
    x_src, c_src = t_src // CORES, lax.rem(t_src, CORES)
    same_x = x == x_src

    up_part = rows // up_steps
    down_part = units // READS

    def up_read(i):
        at = pl.ds(i * up_part, up_part)
        return pltpu.make_async_copy(up_w.at[at, :], up_f.at[at, :], in_sem.at[2 + i])

    def down_read(i):
        at = pl.ds(i * down_part, down_part)
        return pltpu.make_async_copy(down_w.at[at, :], down_f.at[at, :], in_sem.at[2 + up_steps + i])

    gain_read = pltpu.make_async_copy(gain, gain_v, in_sem.at[0])
    prompt_read = pltpu.make_async_copy(prompt, prompt_v, in_sem.at[1])
    gain_read.start()
    up_read(0).start()
    prompt_read.start()
    for i in range(1, up_steps):
        up_read(i).start()
    for i in range(READS):
        down_read(i).start()

    barrier = pltpu.get_barrier_semaphore()
    peers = [sibling]
    peers += [(y, lax.rem(z + d, fs_count), x * CORES + cc) for d in range(1, fs_count) for cc in range(CORES)]
    peers += [(y, z, lax.rem(x + d, chips) * CORES + cc) for d in range(1, chips) for cc in range(CORES)]
    peers += [(lax.rem(y + g, groups), z, t) for g in range(1, groups)]
    for peer in peers:
        pl.semaphore_signal(barrier, inc=1, device_id=peer, device_id_type=MESH)

    gain_read.wait()
    gain_col[...] = jnp.broadcast_to(gain_v[...], (LANES, rows)).T
    step = min(16, up_part)

    def cast_up(n):
        up_read(n).wait()

        @pl.loop(0, up_part // step)
        def _(i):
            at = pl.ds(pl.multiple_of(n * up_part + i * step, step), step)
            factor = gain_col[at, :]
            for j in range(ratio):
                for b in range(units // LANES):
                    piece = up_f[at, j * units + b * LANES : j * units + (b + 1) * LANES]
                    ub[j, at, b * LANES : (b + 1) * LANES] = (factor * piece).astype(jnp.bfloat16)

    cast_up(0)
    pl.semaphore_wait(barrier, len(peers))

    def remote(src, dst, ssem, rsem, dev):
        return pltpu.make_async_remote_copy(
            src_ref=src, dst_ref=dst, send_sem=ssem, recv_sem=rsem, device_id=dev, device_id_type=MESH
        )

    def n_at(zr):
        return nall.at[pl.ds(pl.multiple_of(zr * tokens, tokens), tokens), :]

    def n_copy(zr, up, first):
        src = nb if first else n_at(zr)
        dev = (y, z + 1 if up else z - 1, t)
        return remote(src, n_at(zr), n_send.at[zr, int(up)], n_recv.at[zr], dev)

    def n_hop(h, act, wait):
        for up in (True, False):
            origin = z - h if up else z + h

            @pl.when(jnp.logical_and(origin >= 0, origin < fs_count))
            def _():
                if wait and h > 0:
                    remote(nb, n_at(origin), n_send.at[origin, int(up)], n_recv.at[origin], sibling).wait_recv()

                @pl.when(z < fs_count - 1 if up else z > 0)
                def _():
                    act(n_copy(origin, up, h == 0))

    def up_at(zr, k):
        return up_v.at[pl.ds(pl.multiple_of(zr * rows + k * chunk, chunk), chunk), :]

    def up_index(m, core, owner):
        return (m * CORES + core) * groups + owner

    def src_at(j, m, cd):
        k = up_index(m, cd, y)
        return ub.at[j, pl.ds(pl.multiple_of(k * chunk, chunk), chunk), :]

    def up_x(j, m, cd, dx):
        dev = (y, z, lax.rem(x + dx, chips) * CORES + c)
        sems = up_send.at[j, dx - 1], stage_recv.at[dx - 1, j, m]
        return remote(src_at(j, m, cd), stage.at[dx - 1, j, m, cd], *sems, dev)

    def up_x_own(j, m, cd, dx):
        dev = (y, z, lax.rem(x + dx, chips) * CORES + cd)
        k = up_index(m, cd, y)
        return remote(src_at(j, m, cd), up_at(z, k), up_send.at[j, dx - 1], up_recv.at[z, m, y], dev)

    def up_x_all(act, steps):
        for m in steps:
            for cd in range(CORES):
                for j in range(ratio):
                    mine = t * ratio + j == z
                    for dx in range(1, chips):
                        @pl.when(mine)
                        def _():
                            act(up_x_own(j, m, cd, dx))

                        @pl.when(jnp.logical_not(mine))
                        def _():
                            act(up_x(j, m, cd, dx))

    def up_z(j, m, cd, dx):
        xs = lax.rem(x + dx, chips)
        src = src_at(j, m, cd) if dx == 0 else stage.at[chips - dx - 1, j, m, cd]
        k = up_index(m, cd, y)
        dev = (y, (xs * CORES + c) * ratio + j, x * CORES + cd)
        return remote(src, up_at(z, k), z_send.at[j, dx], up_recv.at[z, m, y], dev)

    def away(j, dx, fn):
        pl.when((lax.rem(x + dx, chips) * CORES + c) * ratio + j != z)(fn)

    def go_z(m, j, dx):
        def go():
            if dx > 0:
                at = stage.at[chips - dx - 1, j, m]
                remote(at, at, up_send.at[j, 0], stage_recv.at[chips - dx - 1, j, m], sibling).wait_recv()
            for cd in range(CORES):
                up_z(j, m, cd, dx).start()

        away(j, dx, go)

    def z_own(m):
        for j in range(ratio):
            go_z(m, j, 0)

    def z_staged(m):
        for j in range(ratio):
            for dx in range(1, chips):
                go_z(m, j, dx)

    def sent(ref, sem):
        remote(ref, ref, sem, own_recv, sibling).wait_send()

    def landed(ref, sem):
        remote(ref, ref, own_send, sem, sibling).wait_recv()

    own_j = lax.rem(z, ratio)
    own_rows = pl.ds(pl.multiple_of(z * rows, rows), rows)
    my_cols = pl.ds(pl.multiple_of(t * width, width), width)

    def own_copy():
        return remote(ub.at[own_j], up_v.at[own_rows, :], own_send, own_recv, sibling)

    def sib_copy():
        return remote(down_v.at[:, my_cols], down_v.at[:, my_cols], sib_send, sib_recv, sibling)

    def cols_of(ts, i):
        return pl.ds(pl.multiple_of(ts * width + i * LANES, LANES), LANES)

    def dn_at(ts, i, k):
        return down_v.at[pl.ds(pl.multiple_of(k * k_rows, k_rows), k_rows), cols_of(ts, i)]

    def dn_col(ts, i):
        return down_v.at[:, cols_of(ts, i)]

    def dn_to(dx):
        return (y, z, lax.rem(x + dx, chips) * CORES + c)

    def dn_sends():
        for i in range(col_chunks):
            for n in range(1 if whole(i) else k_pieces // groups):
                for dx in range(1, chips):
                    if whole(i):
                        at, sem = dn_col(t, i), dn_recv.at[dx - 1, i, 0]
                    else:
                        at, sem = dn_at(t, i, n * groups + y), dn_recv.at[dx - 1, i, n * groups + y]
                    remote(at, at, dn_send.at[int(whole(i)), dx - 1], sem, dn_to(dx)).start()

    start = lambda copy: copy.start()
    prompt_read.wait()
    widened = prompt_v[...].astype(jnp.float32)
    scale = lax.rsqrt(jnp.mean(widened * widened, axis=-1, keepdims=True) + epsilon)
    nb[...] = (widened * scale).astype(jnp.bfloat16)
    def feed(m):
        if m + 1 < up_steps:
            cast_up(m + 1)
        up_x_all(start, (m,))
        if m < AHEAD:
            z_own(m)

    up_x_all(start, (0,))
    z_own(0)
    n_hop(0, start, False)
    if up_steps > 1:
        cast_up(1)

    down_step = min(64, down_part)

    def cast_down(n):
        down_read(n).wait()

        @pl.loop(0, down_part // down_step)
        def _(i):
            at = pl.ds(pl.multiple_of(n * down_part + i * down_step, down_step), down_step)
            down_v[at, my_cols] = down_f[at, :].astype(jnp.bfloat16)

    def start_down():
        dn_sends()
        sib_copy().start()

    def keep_own():
        n_at(z)[...] = nb[...]

        @pl.when(t == t_src)
        def _():
            own_copy().start()

            @pl.loop(0, rows // chunk)
            def _(i):
                part = pl.ds(pl.multiple_of(i * chunk, chunk), chunk)
                up_v[pl.ds(pl.multiple_of(z * rows + i * chunk, chunk), chunk), :] = ub[own_j, part, :]

    def up_y(zr, m, g):
        dev = (lax.rem(y + g, groups), z, t)
        at = up_at(zr, up_index(m, c, y))
        return remote(at, at, upf_send.at[zr, g], up_recv.at[zr, m, y], dev)

    def up_s(zr, m, owner):
        at = up_at(zr, up_index(m, c, owner))
        return remote(at, at, upf_send.at[zr, 0], up_sib.at[zr], sibling)

    def up_in(zr, m, owner):
        landed(up_at(zr, up_index(m, c, owner)), up_recv.at[zr, m, owner])

    def if_remote(d, fn):
        if d == 0:
            pl.when(jnp.logical_not(same_x))(fn)
        else:
            fn()

    def source(d):
        if d == 0 or fs_count > 8:
            return lax.rem(z + d, fs_count)
        found = 0
        for at in range(fs_count):
            order = sorted((o for o in range(fs_count) if o != at), key=lambda o: rank(o, at, fs_count))
            found = jnp.where(z == at, order[d - 1], found)
        return found

    def up_a(m, d):
        def go():
            zr = source(d)
            up_in(zr, m, y)
            for g in range(1, groups):
                up_y(zr, m, g).start()
            up_s(zr, m, y).start()

        if_remote(d, go)

    def up_b(m, d):
        def go():
            zr = source(d)
            for g in range(1, groups):
                owner = lax.rem(y + g, groups)
                up_in(zr, m, owner)
                up_s(zr, m, owner).start()

        if_remote(d, go)

    def up_c(d):
        if_remote(d, lambda: landed(up_v.at[pl.ds(0, rows // CORES), :], up_sib.at[source(d)]))

    def up_done(d):
        def go():
            zr = source(d)
            sent(up_v.at[pl.ds(0, rows // CORES), :], upf_send.at[zr, 0])
            for g in range(1, groups):
                sent(up_v.at[pl.ds(0, rows // (CORES * groups)), :], upf_send.at[zr, g])

        if_remote(d, go)

    def dn_src(dx):
        return lax.rem(x + dx, chips) * CORES + c

    def dn_whole(i, dx):
        at = dn_col(dn_src(dx), i)
        landed(at, dn_recv.at[chips - dx - 1, i, 0])
        remote(at, at, dnf_send.at[dx - 1, 0], dn_sib.at[dx - 1, i], sibling).start()

    def dn_piece(i, k, dx, forward):
        at, sem = dn_at(dn_src(dx), i, k), dn_recv.at[chips - dx - 1, i, k]
        landed(at, sem)
        if forward:
            for g in range(1, groups):
                remote(at, at, dnf_send.at[dx - 1, g], sem, (lax.rem(y + g, groups), z, t)).start()
        remote(at, at, dnf_send.at[dx - 1, 0], dn_sib.at[dx - 1, i], sibling).start()

    def dn_a(i, n, dx):
        dn_piece(i, n * groups + y, dx, True)

    def dn_b(i, n, dx):
        for g in range(1, groups):
            dn_piece(i, n * groups + lax.rem(y + g, groups), dx, False)

    part = functools.partial
    events, queued = [], []
    for m in range(1, up_steps):
        events.append((FEED * m, part(feed, m)))
    for n in range(READS):
        events.append((DOWN_CAST + 0.03 * n, part(cast_down, n)))
    events.append((DOWN_CAST + 0.03 * READS, start_down))
    events.append((DOWN_CAST + 0.03 * READS + 0.05, keep_own))
    for m in range(up_steps):
        share = m / max(1, up_steps - 1)
        when = STAGE[0] + (STAGE[1] - STAGE[0]) * share
        events.append((when, part(z_staged, m)))
        if m + AHEAD < up_steps:
            events.append((when + 0.001, part(z_own, m + AHEAD)))
        for d in range(fs_count):
            base, span = ARRIVAL[min(d, len(ARRIVAL) - 1)]
            when = max(base + (span - base) * share, STAGE[0] + (STAGE[1] - STAGE[0]) * share + 0.01) + 0.002 * d
            events.append((when, part(up_a, m, d)))
            events.append((when + LAG_Y, part(up_b, m, d)))
    for h in range(1, fs_count):
        when = ROWS[h - 1] if h <= len(ROWS) else 1.2 + h
        events.append((when, part(n_hop, h, start, True)))
    for i in range(lead):
        for dx in range(1, chips):
            events.append((1.1, part(dn_whole, i, dx)))
    for i in split:
        for n in range(k_pieces // groups):
            for dx in range(1, chips):
                events.append((DOWN_TURN + 0.001 * i, part(dn_a, i, n, dx)))
    for _, event in sorted(events, key=lambda e: e[0]):
        event()

    for d in range(fs_count):
        up_c(d)

    @pl.when(jnp.logical_and(same_x, t != t_src))
    def _():
        own_copy().wait_recv()

    depth = prompt.shape[1]
    kb = 256
    nb_tile = min(units, 1024)

    pieces = depth // kb
    for i in range(pieces):
        for j in range(units // nb_tile):
            col = pl.ds(j * nb_tile, nb_tile)
            term = jnp.dot(
                nall[:, i * kb : (i + 1) * kb],
                up_v[i * kb : (i + 1) * kb, col],
                preferred_element_type=jnp.float32,
            )
            if i == 0:
                proj[:, col] = term
            else:
                proj[:, col] += term

    positive = jnp.maximum(proj[...], 0.0)
    hidden[...] = (positive * positive).astype(jnp.bfloat16)

    def r_copy(ts, i, wide, d):
        zt = lax.rem(z + d, fs_count)
        cols = pl.ds(pl.multiple_of(ts * width + i * LANES, LANES), wide)
        return remote(pbuf.at[zt, :, cols], rbuf.at[z, :, cols], r_send.at[d], r_recv.at[z], (y, zt, t))

    def block(ts, i, wide):
        cols = pl.ds(pl.multiple_of(ts * width + i * LANES, LANES), wide)
        part = jnp.dot(hidden[...], down_v[:, cols], preferred_element_type=jnp.float32).astype(jnp.bfloat16)
        pbuf[:, :, cols] = part.reshape(fs_count, tokens, wide)

    blocks = [(t, 0, width), (x * CORES + 1 - c, 0, width)]
    for i in range(col_chunks):
        for dx in range(1, chips):
            blocks += [(dn_src(dx), i, LANES), (lax.rem(x + dx, chips) * CORES + 1 - c, i, LANES)]

    def send_block(ts, i, wide):
        for d in range(1, fs_count):
            r_copy(ts, i, wide, d).start()

    last = None
    for index, (ts, i, wide) in enumerate(blocks):
        if index == 1:
            sib_copy().wait_recv()
        if index >= CORES:
            dx = 1 + (index - CORES) // CORES % (chips - 1)
            if (index - CORES) % CORES == 0 and whole(i) and i >= lead:
                dn_whole(i, dx)
            if (index - CORES) % CORES == 0 and not whole(i):
                for n in range(k_pieces // groups):
                    dn_b(i, n, dx)
            if (index - CORES) % CORES == 1:
                landed(dn_col(ts, i), dn_sib.at[dx - 1, i])
        block(ts, i, wide)
        if last is not None:
            send_block(*last)
        last = (ts, i, wide)
    send_block(*last)

    total = pbuf[z].astype(jnp.float32)

    @pl.loop(1, fs_count)
    def _(d):
        zr = lax.rem(z + d, fs_count)
        remote(pbuf.at[zr], rbuf.at[zr], r_send.at[d], r_recv.at[zr], (y, zr, t)).wait()

    for d in range(1, fs_count):
        total += rbuf[lax.rem(z + d, fs_count)].astype(jnp.float32)
    out_v[...] = total.astype(jnp.bfloat16)

    for d in range(fs_count):
        up_done(d)
    for dx in range(1, chips):
        sent(down_v.at[:, pl.ds(0, width)], dnf_send.at[dx - 1, 0])
        if whole_cols > 0:
            sent(down_v.at[:, pl.ds(0, whole_cols * LANES)], dn_send.at[1, dx - 1])
        if whole_cols < col_chunks:
            half = down_v.at[pl.ds(0, units // groups), pl.ds(0, (col_chunks - whole_cols) * LANES)]
            sent(half, dn_send.at[0, dx - 1])
            for g in range(1, groups):
                sent(half, dnf_send.at[dx - 1, g])
    for j in range(ratio):
        half = up_v.at[pl.ds(0, rows // groups), :]
        for dx in range(1, chips):
            sent(half, up_send.at[j, dx - 1])
        for dx in range(chips):
            away(j, dx, functools.partial(sent, half, z_send.at[j, dx]))
    sib_copy().wait_send()

    @pl.when(t == t_src)
    def _():
        own_copy().wait_send()

    for h in range(fs_count):
        n_hop(h, lambda copy: copy.wait_send(), False)


def write_out(up_v, down_v, out_v, up_out, down_out, mlp_out, sems):
    copies = [pltpu.make_async_copy(out_v, mlp_out, sems.at[2 * PIECES])]
    for n, (src, dst) in enumerate(((up_v, up_out), (down_v, down_out))):
        step = src.shape[0] // PIECES
        for i in range(PIECES):
            part = pl.ds(i * step, step)
            copies.append(pltpu.make_async_copy(src.at[part, :], dst.at[part, :], sems.at[n * PIECES + i]))
    for copy in copies:
        copy.start()
    for copy in copies:
        copy.wait()


def per_device(groups, prompt, norm_gain, up_weight, down_weight):
    tp_count, fs_count = lax.axis_size("tp"), lax.axis_size("fs")
    rows, wide = up_weight.shape
    units, width = down_weight.shape
    tokens, depth = prompt.shape
    ratio = wide // units
    up_steps = max(1, min(UP_STEPS, rows // (CORES * groups * 16)))
    col_chunks = width // LANES
    whole_cols = int(col_chunks * WHOLE_PART)
    chips = tp_count // CORES
    kc = up_steps * CORES * groups
    k_pieces = K_PIECES
    f32, bf16 = jnp.float32, jnp.bfloat16
    dma = pltpu.SemaphoreType.DMA
    vmem = pl.BlockSpec(memory_space=pltpu.VMEM)
    hbm = pl.BlockSpec(memory_space=pltpu.HBM)
    up_v, down_v, out_v = pl.pallas_call(
        functools.partial(kernel, groups, fs_count, tp_count, up_steps, whole_cols, k_pieces),
        out_shape=(
            pltpu.VMEM((depth, units), bf16),
            pltpu.VMEM((units, depth), bf16),
            pltpu.VMEM((tokens, depth), bf16),
        ),
        in_specs=[hbm] * 4,
        out_specs=(vmem,) * 3,
        scratch_shapes=[
            pltpu.VMEM((1, rows), f32),
            pltpu.VMEM((tokens, depth), bf16),
            pltpu.VMEM((rows, wide), f32),
            pltpu.VMEM((units, width), f32),
            pltpu.VMEM((rows, LANES), f32),
            pltpu.VMEM((ratio, rows, units), bf16),
            pltpu.VMEM((tokens, depth), bf16),
            pltpu.VMEM((fs_count * tokens, depth), bf16),
            pltpu.VMEM((fs_count * tokens, units), f32),
            pltpu.VMEM((fs_count * tokens, units), bf16),
            pltpu.VMEM((fs_count, tokens, depth), bf16),
            pltpu.VMEM((fs_count, tokens, depth), bf16),
            pltpu.VMEM((chips - 1, ratio, up_steps, CORES, rows // kc, units), bf16),
            dma((2 + up_steps + READS,)),
            dma((ratio, chips - 1)),
            dma((chips - 1, ratio, up_steps)),
            dma((ratio, chips)),
            dma((fs_count, up_steps, groups)),
            dma((fs_count,)),
            dma((fs_count, groups)),
            dma, dma,
            dma((2, chips - 1)),
            dma((chips - 1, col_chunks, k_pieces)),
            dma((chips - 1, col_chunks)),
            dma((chips - 1, groups)),
            dma, dma,
            dma((fs_count, 2)),
            dma((fs_count,)),
            dma((fs_count,)),
            dma((fs_count,)),
        ],
        compiler_params=pltpu.CompilerParams(
            collective_id=0, has_side_effects=True, vmem_limit_bytes=40 * 1024 * 1024
        ),
    )(norm_gain.reshape(1, rows), up_weight, down_weight, prompt)
    any_space = pl.BlockSpec(memory_space=pl.ANY)
    return pl.pallas_call(
        write_out,
        out_shape=(
            jax.ShapeDtypeStruct(up_v.shape, bf16),
            jax.ShapeDtypeStruct(down_v.shape, bf16),
            jax.ShapeDtypeStruct(out_v.shape, bf16),
        ),
        in_specs=[vmem] * 3,
        out_specs=(any_space,) * 3,
        scratch_shapes=[dma((2 * PIECES + 1,))],
        compiler_params=pltpu.CompilerParams(vmem_limit_bytes=1024 * 1024),
        cost_estimate=pl.CostEstimate(flops=0, bytes_accessed=4 * depth * units * 2, transcendentals=0),
    )(up_v, down_v, out_v)


def solution(mesh):
    return jax.shard_map(
        functools.partial(per_device, mesh.shape["grp"]),
        mesh=mesh,
        in_specs=(P(("grp", "fs", "tp"), None), P("fs"), P("fs", "tp"), P("fs", "tp")),
        out_specs=(P("grp", "fs"), P("fs", "grp"), P(("grp", "fs", "tp"), None)),
        check_vma=False,
    )
```
